32 devices in a mesh: dp: 4 (over y, x), kv: 4 (over z), tp: 2 (over core).
Axes of the slice: x: 2, y: 2, z: 4, core: 2. Of those that a mesh axis runs over, the one named last changes fastest.
Arguments:
- tokens: bfloat16 [16, 4096], P('dp', 'kv'), may hold values from -18 to 18
- norm_gain: float32 [4096], P('kv'), may hold values from 0.1 to 1.9
- query_weight: bfloat16 [4096, 4096], P('kv', 'tp'), may hold values from -0.09375 to 0.09375
- key_weight: bfloat16 [4096, 512], P('kv', 'tp'), may hold values from -0.09375 to 0.09375
- value_weight: bfloat16 [4096, 512], P('kv', 'tp'), may hold values from -0.09375 to 0.09375
- gate_weight: bfloat16 [4096, 8], replicated, may hold values from -0.09375 to 0.09375
- gate_bias: float32 [8], replicated, may hold values from -2.5 to 0.5
- query_gain: float32 [64], replicated, may hold values from 0.1 to 1.9
- key_gain: float32 [64], replicated, may hold values from 0.1 to 1.9
- key_cache: bfloat16 [16, 8192, 512], P('dp', 'kv', 'tp'), may hold values from -6 to 6
- value_cache: bfloat16 [16, 8192, 512], P('dp', 'kv', 'tp'), may hold values from -9 to 9
- gate_cache: float32 [16, 8, 8192], P('dp', 'tp', 'kv'), may hold values from -8192 to 0, as said below
- lengths: int32 [16], P('dp'), may hold values from 4097 to 8192, as said below
- out_weight: bfloat16 [4096, 4096], P('tp', 'kv'), may hold values from -0.75 to 0.75
Outputs:
- mixed: bfloat16 [16, 4096], P('dp', 'kv')
The draws below stay inside these ranges and needn't reach their ends.
Inputs may be any that keep to these rules, and one draw needn't show every extreme that they name: `gate_cache`: never rising along positions. `lengths`: in every draw some sequence has all 8192 positions cached.
All inputs are finite; a program needn't handle non-finite values.
Results may differ from the reference program's by a relative error of at most 0.012.
Values may be sent and summed in bfloat16 or wider, within the bound.
A program may use at most 64 MiB of HBM per device.

```python
import math
import jax
import jax.numpy as jnp
from jax import lax

D = 4096
HEADS = 64
KV_HEADS = 8
HEAD = 64
POS_DEV = 2048
BATCH = 16
SPAN = 8192
N_KV = 4
N_TP = 2


def draw_tokens(key, part):
    first, second, third = jax.random.split(key, 3)
    width = max(D // 32, 1)
    base = jnp.clip(jax.random.normal(first, (BATCH, D), jnp.float32), -6.0, 6.0)
    scales = jnp.exp(jax.random.uniform(second, (BATCH, D // width), jnp.float32, -1.09, 1.09))
    return (base * jnp.repeat(scales, width, axis=1)).astype(jnp.bfloat16)


def draw_value_cache(key, part):
    first, second = jax.random.split(key, 2)
    channels = KV_HEADS * HEAD
    block = max(POS_DEV // 4, 1)
    blocks = SPAN // block
    offsets = jnp.clip(jax.random.normal(second, (BATCH, blocks, 1, channels), jnp.float32), -3.0, 3.0)
    base = jnp.clip(jax.random.normal(first, (BATCH, blocks, block, channels), jnp.float32), -6.0, 6.0)
    return (base + offsets).reshape(BATCH, SPAN, channels).astype(jnp.bfloat16)


def draw_gate_cache(key, part):
    keys = jax.random.split(key, 6)
    share = 0.5
    flags = jax.random.uniform(keys[0], (BATCH, KV_HEADS), jnp.float32) < share
    forced = jax.random.randint(keys[1], (), 0, BATCH * KV_HEADS)
    flags = flags | (jnp.arange(BATCH * KV_HEADS).reshape(BATCH, KV_HEADS) == forced)
    fast = jnp.exp(jax.random.uniform(keys[2], (BATCH, KV_HEADS), jnp.float32, math.log(0.01), math.log(0.033)))
    slow = jnp.exp(jax.random.uniform(keys[3], (BATCH, KV_HEADS), jnp.float32, math.log(0.3), math.log(1.5))) / SPAN
    rate = jnp.where(flags, fast, slow)
    block = max(POS_DEV // 2, 1)
    blocks = SPAN // block
    factor = jnp.exp(jax.random.uniform(keys[4], (BATCH, KV_HEADS, blocks, 1), jnp.float32, math.log(0.35), math.log(2.8)))
    rough = jax.random.uniform(keys[5], (BATCH, KV_HEADS, blocks, block), jnp.float32, 0.5, 1.5)
    steps = -(rate[:, :, None, None] * factor * rough).reshape(BATCH, KV_HEADS, SPAN)
    return jnp.cumsum(steps, axis=2)


def draw_lengths(key, part):
    first, second = jax.random.split(key, 2)
    lengths = SPAN - jax.random.randint(first, (BATCH,), 0, SPAN // 2)
    chosen = jax.random.randint(second, (), 0, BATCH)
    return jnp.where(jnp.arange(BATCH) == chosen, SPAN, lengths).astype(jnp.int32)


def level_of(rng, extent, cuts, low, top_value):
    level, own = 1.0, jax.random.fold_in(rng, 6)
    for dim, shards_of in cuts:
        draws = jnp.exp(jax.random.uniform(jax.random.fold_in(own, dim), (shards_of,), jnp.float32, low / len(cuts), top_value / len(cuts)))
        level = level * jnp.repeat(draws, extent[dim] // shards_of).reshape([-1 if axis == dim else 1 for axis in range(len(extent))])
    return level


def bell_draw(own_key, dims, spread, limit, cuts=(), kind=jnp.bfloat16):
    level = level_of(own_key, dims, cuts, -0.22, 0.18) if cuts else 1.0
    array = jax.random.normal(own_key, dims, jnp.float32) * spread * level
    return jnp.minimum(jnp.maximum(array, -limit), limit).astype(kind)


def setup_inputs(seed: int = 0) -> dict:
    key_of = jax.random.split(jax.random.key(seed), 15)
    return {
        "tokens": draw_tokens(jax.random.fold_in(key_of[14], 71), 0),
        "norm_gain": jnp.clip(1.0 + 0.18 * jax.random.normal(key_of[1], (D,), jnp.float32), 0.1, 1.9),
        "query_weight": bell_draw(key_of[2], (D, HEADS * HEAD), D ** -0.5, 0.09375, ((0, 4), (1, 2))),
        "key_weight": bell_draw(key_of[3], (D, KV_HEADS * HEAD), D ** -0.5, 0.09375, ((0, 4), (1, 2))),
        "value_weight": bell_draw(key_of[4], (D, KV_HEADS * HEAD), D ** -0.5, 0.09375, ((0, 4), (1, 2))),
        "gate_weight": bell_draw(key_of[5], (D, KV_HEADS), D ** -0.5, 0.09375),
        "gate_bias": jnp.clip(jax.random.uniform(key_of[6], (KV_HEADS,), jnp.float32, -2.5, 0.5), -2.5, 0.5),
        "query_gain": jnp.clip(1.0 + 0.18 * jax.random.normal(key_of[7], (HEAD,), jnp.float32), 0.1, 1.9),
        "key_gain": jnp.clip(1.0 + 0.18 * jax.random.normal(key_of[8], (HEAD,), jnp.float32), 0.1, 1.9),
        "key_cache": bell_draw(key_of[9], (BATCH, SPAN, KV_HEADS * HEAD), 1.0, 6.0, ((0, 4), (1, 4), (2, 2))),
        "value_cache": draw_value_cache(jax.random.fold_in(key_of[14], 71), 0),
        "gate_cache": draw_gate_cache(jax.random.fold_in(key_of[14], 71), 0),
        "lengths": draw_lengths(jax.random.fold_in(key_of[14], 71), 0),
        "out_weight": bell_draw(key_of[13], (HEADS * HEAD, D), HEAD ** -0.5, 0.75, ((0, 2), (1, 4))),
    }


EPSILON = 1e-06
FLOOR = -1e+30

def head_norm(values, gain):
    values = values.astype(jnp.float32)
    return values * lax.rsqrt(lax.optimization_barrier(jnp.mean(values * values, axis=-1, keepdims=True)) + EPSILON) * gain

def one_sequence(inputs):
    queries, key_new, value_new, log_gate, key_rows, value_rows, gate_rows, length = inputs
    scale = HEAD ** (-0.5)
    keys = key_rows.reshape(N_KV, POS_DEV, KV_HEADS, HEAD).astype(jnp.float32)
    values = value_rows.reshape(N_KV, POS_DEV, KV_HEADS, HEAD).astype(jnp.float32)
    gates = gate_rows.reshape(KV_HEADS, N_KV, POS_DEV).transpose(1, 0, 2)
    queries_f = queries.astype(jnp.float32)
    scores = jnp.einsum('grd,bpgd->bgrp', queries_f, keys) * scale - gates[:, :, None, :]
    places = jnp.arange(SPAN, dtype=jnp.int32).reshape(N_KV, POS_DEV)
    live = (places < length)[:, None, None, :]
    last = (length - 1).astype(jnp.int32)
    last_gate = lax.dynamic_slice_in_dim(gate_rows, last, 1, 1)[:, 0]
    own_gate = last_gate + log_gate
    score_new = jnp.einsum('grd,gd->gr', queries_f, key_new.astype(jnp.float32)) * scale - own_gate[:, None]
    owner = (jnp.arange(N_KV, dtype=jnp.int32) == last // POS_DEV)[:, None, None]
    block_max = lax.optimization_barrier(jnp.max(jnp.where(live, scores, FLOOR), axis=3))
    block_max = jnp.where(owner, jnp.maximum(block_max, score_new[None]), block_max)
    weights = jnp.where(live, jnp.exp(scores - block_max[..., None]), 0.0).astype(jnp.bfloat16)
    weights = lax.optimization_barrier(weights).astype(jnp.float32)
    weight_new = jnp.where(owner, jnp.exp(score_new[None] - block_max), 0.0).astype(jnp.bfloat16)
    weight_new = lax.optimization_barrier(weight_new).astype(jnp.float32)
    block_sum = lax.optimization_barrier(jnp.sum(weights, axis=3)) + weight_new
    block_values = jnp.einsum('bgrp,bpgd->bgrd', weights, values)
    block_values = block_values + weight_new[..., None] * value_new.astype(jnp.float32)[None, :, None, :]
    top = lax.optimization_barrier(jnp.max(block_max, axis=0))
    factor = jnp.exp(block_max - top)
    total = lax.optimization_barrier(jnp.sum(factor * block_sum, axis=0))
    summed = lax.optimization_barrier(jnp.sum(factor[..., None] * block_values, axis=0))
    return (summed / total[..., None]).astype(jnp.bfloat16).reshape(HEADS * HEAD)

def reference(tokens, norm_gain, query_weight, key_weight, value_weight, gate_weight, gate_bias, query_gain, key_gain, key_cache, value_cache, gate_cache, lengths, out_weight):
    count = tokens.shape[0]
    ratio = HEADS // KV_HEADS
    tokens_f = tokens.astype(jnp.float32)
    inverse = lax.rsqrt(lax.optimization_barrier(jnp.sum(tokens_f * tokens_f, axis=1)) / D + EPSILON)[:, None]
    scaled = (tokens_f * norm_gain).astype(jnp.bfloat16)
    query_raw = (jnp.dot(scaled, query_weight, preferred_element_type=jnp.float32) * inverse).astype(jnp.bfloat16)
    key_raw = (jnp.dot(scaled, key_weight, preferred_element_type=jnp.float32) * inverse).astype(jnp.bfloat16)
    value_new = (jnp.dot(scaled, value_weight, preferred_element_type=jnp.float32) * inverse).astype(jnp.bfloat16)
    log_gate = jax.nn.log_sigmoid(jnp.dot(scaled, gate_weight, preferred_element_type=jnp.float32) * inverse + gate_bias)
    queries = head_norm(query_raw.reshape(count, KV_HEADS, ratio, HEAD), query_gain).astype(jnp.bfloat16)
    key_new = head_norm(key_raw.reshape(count, KV_HEADS, HEAD), key_gain).astype(jnp.bfloat16)
    attended = lax.map(one_sequence, (queries, key_new, value_new.reshape(count, KV_HEADS, HEAD), log_gate, key_cache, value_cache, gate_cache, lengths))
    rows = HEADS * HEAD // N_TP
    total = jnp.zeros((count, D), jnp.float32)
    for group in range(N_TP):
        part = jnp.dot(attended[:, group * rows:(group + 1) * rows], out_weight[group * rows:(group + 1) * rows], preferred_element_type=jnp.float32).astype(jnp.bfloat16)
        total = total + lax.optimization_barrier(part).astype(jnp.float32)
    return total.astype(jnp.bfloat16)
```

```python
import functools

import jax
import jax.numpy as jnp
from jax import lax
from jax.experimental import pallas as pl
from jax.experimental.pallas import tpu as pltpu
from jax.sharding import PartitionSpec as P

EPSILON = 1e-06
FLOOR = -1e30
LANES = 128
CHUNKS = 4
MESH = pl.DeviceIdType.MESH
F32 = jnp.float32
BF16 = jnp.bfloat16


def kernel(
    dims,
    tokens,
    norm_gain,
    query_weight,
    key_weight,
    value_weight,
    gate_weight,
    gate_bias,
    query_gain,
    key_gain,
    key_cache,
    value_cache,
    gate_cache,
    lengths,
    out_weight,
    out,
    qw,
    kw,
    vw,
    gw,
    keys,
    values,
    gates,
    ow,
    part,
    bias,
    heads_q,
    heads_o,
    mixed_in,
    sums,
    blocks,
    stats,
    halves,
    local_sem,
    send_sum,
    recv_sum,
    send_block,
    recv_block,
    send_stat,
    recv_stat,
    half_sem,
):
    n_kv, n_tp, width, head = dims
    kv = lax.axis_index("kv")
    tp = lax.axis_index("tp")
    seqs, columns = tokens.shape
    positions = keys.shape[1]
    q_chunk = qw.shape[2]
    q_rows = query_weight.shape[1] // LANES
    k_width = key_weight.shape[1]
    k_rows = k_width // LANES
    groups = k_width // head
    n_heads = query_weight.shape[1] // head
    ratio = n_heads // groups
    k_base = seqs * q_rows
    v_base = k_base + seqs * k_rows
    g_base = v_base + seqs * k_rows
    gate_columns = gate_weight.shape[0]

    barrier = pltpu.get_barrier_semaphore()
    for step in range(1, n_kv):
        peer = lax.rem(kv + step, n_kv)
        pl.semaphore_signal(barrier, inc=1, device_id={"kv": peer}, device_id_type=MESH)
    for step in range(1, n_tp):
        peer = lax.rem(tp + step, n_tp)
        pl.semaphore_signal(barrier, inc=1, device_id={"tp": peer}, device_id_type=MESH)

    loads = []

    def load(src, dst):
        copy = pltpu.make_async_copy(src, dst, local_sem.at[len(loads)])
        copy.start()
        loads.append(copy)
        return copy

    row_start = pl.multiple_of(kv * columns, LANES)
    load_q = [
        load(query_weight.at[:, pl.ds(i * q_chunk, q_chunk)], qw.at[i]) for i in range(CHUNKS)
    ]
    load_k = load(key_weight, kw)
    load_v = load(value_weight, vw)
    load_g = load(gate_weight.at[:, pl.ds(row_start, columns)], gw)
    load_gates = load(gate_cache, gates)
    load_keys = [load(key_cache.at[s], keys.at[s]) for s in range(seqs)]
    load_values = [load(value_cache.at[s], values.at[s]) for s in range(seqs)]
    load_out = load(out_weight, ow)

    tokens_f = tokens[...].astype(F32)
    squares = jnp.sum(tokens_f * tokens_f, axis=1, keepdims=True)
    scaled = (tokens_f * norm_gain[...]).astype(BF16)
    for i in range(CHUNKS):
        load_q[i].wait()
        product = jnp.dot(scaled, qw[i], preferred_element_type=F32)
        for j in range(q_chunk // LANES):
            row = i * (q_chunk // LANES) + j
            part[pl.ds(row, seqs, stride=q_rows), :] = product[:, j * LANES : (j + 1) * LANES]
    for copy, weight, base in ((load_k, kw, k_base), (load_v, vw, v_base)):
        copy.wait()
        product = jnp.dot(scaled, weight[...], preferred_element_type=F32)
        for j in range(k_rows):
            part[pl.ds(base + j, seqs, stride=k_rows), :] = product[:, j * LANES : (j + 1) * LANES]
    load_g.wait()
    part[g_base:, :] = jnp.zeros((part.shape[0] - g_base, LANES), F32)
    part[g_base : g_base + seqs, :gate_columns] = lax.dot_general(
        scaled, gw[...], (((1,), (1,)), ((), ())), preferred_element_type=F32
    )
    part[g_base : g_base + seqs, gate_columns : gate_columns + 1] = squares
    sums[kv] = part[...].astype(BF16)

    pl.semaphore_wait(barrier, n_kv + n_tp - 2)

    def spread(ref, send, recv):
        copies = []
        for step in range(1, n_kv):
            peer = lax.rem(kv + step, n_kv)
            copy = pltpu.make_async_remote_copy(
                src_ref=ref.at[kv],
                dst_ref=ref.at[kv],
                send_sem=send.at[step],
                recv_sem=recv.at[kv],
                device_id={"kv": peer},
                device_id_type=MESH,
            )
            copy.start()
            copies.append(copy)
        return copies

    def arrive(ref, send, recv):
        for step in range(1, n_kv):
            peer = lax.rem(kv + n_kv - step, n_kv)
            pltpu.make_async_remote_copy(
                src_ref=ref.at[peer],
                dst_ref=ref.at[peer],
                send_sem=send.at[step],
                recv_sem=recv.at[peer],
                device_id={"kv": peer},
                device_id_type=MESH,
            ).wait_recv()

    sent = spread(sums, send_sum, recv_sum)

    lane = lax.broadcasted_iota(jnp.int32, (1, LANES), 1)
    low = lane < head
    places = lax.broadcasted_iota(jnp.int32, (groups, positions), 1)
    load_gates.wait()
    last_gates = []
    for s in range(seqs):
        within = lengths[s] - 1 - kv * positions
        gate = gates[s]
        bias[s] = jnp.where(places <= within, -gate, FLOOR)
        last_gates.append(
            jnp.sum(jnp.where(places == within, gate, 0.0), axis=1, keepdims=True)
        )
    bias_row = jnp.zeros((1, LANES), F32)
    for j in range(gate_columns):
        bias_row = jnp.where(lane == j, gate_bias[j], bias_row)
    q_gain = jnp.concatenate([query_gain[...]] * (LANES // head), axis=1)
    k_gain = jnp.concatenate([key_gain[...]] * (LANES // head), axis=1)

    def head_norm(raw, gain):
        square = raw * raw
        first = jnp.sum(jnp.where(low, square, 0.0), axis=1, keepdims=True)
        second = jnp.sum(jnp.where(low, 0.0, square), axis=1, keepdims=True)
        factor = jnp.where(
            low, lax.rsqrt(first / head + EPSILON), lax.rsqrt(second / head + EPSILON)
        )
        return (raw * factor * gain).astype(BF16).astype(F32)

    def swap(x):
        return pltpu.roll(x, head, 1)

    head_row = lax.broadcasted_iota(jnp.int32, (n_heads, k_width), 0)
    head_lane = lax.broadcasted_iota(jnp.int32, (n_heads, k_width), 1)
    own_group = (head_row // ratio) == (head_lane // head)
    stat_row = lax.broadcasted_iota(jnp.int32, (n_heads, LANES), 0)
    stat_lane = lax.broadcasted_iota(jnp.int32, (n_heads, LANES), 1)

    arrive(sums, send_sum, recv_sum)
    total = sums[0].astype(F32)
    for i in range(1, n_kv):
        total = total + sums[i].astype(F32)
    tail = total[g_base : g_base + seqs]
    square_sum = jnp.sum(jnp.where(lane == gate_columns, tail, 0.0), axis=1, keepdims=True)
    inverse = lax.rsqrt(square_sum / width + EPSILON)
    logits = tail * inverse + bias_row
    log_gate = jnp.minimum(logits, 0.0) - jnp.log1p(jnp.exp(-jnp.abs(logits)))

    max_row = jnp.zeros((1, LANES), F32)
    sum_row = jnp.zeros((1, LANES), F32)
    for s in range(seqs):
        inv = inverse[s : s + 1]
        raw = (total[s * q_rows : (s + 1) * q_rows] * inv).astype(BF16).astype(F32)
        query = head_norm(raw, q_gain) * (head ** -0.5)
        turned = swap(query)
        heads_q[s, pl.ds(0, q_rows, stride=2), :] = jnp.where(low, query, turned)
        heads_q[s, pl.ds(1, q_rows, stride=2), :] = jnp.where(low, turned, query)
        key_raw = total[k_base + s * k_rows : k_base + (s + 1) * k_rows] * inv
        key_new = head_norm(key_raw.astype(BF16).astype(F32), k_gain)
        value_new = (
            (total[v_base + s * k_rows : v_base + (s + 1) * k_rows] * inv)
            .astype(BF16)
            .astype(F32)
        )
        key_row = jnp.concatenate([key_new[j : j + 1] for j in range(k_rows)], axis=1)
        value_row = jnp.concatenate([value_new[j : j + 1] for j in range(k_rows)], axis=1)
        spread_q = jnp.where(
            own_group, jnp.concatenate([heads_q[s]] * k_rows, axis=1), 0.0
        )
        score_new = jnp.sum(spread_q * key_row, axis=1, keepdims=True)
        own_gate = []
        for g in range(groups):
            gate = last_gates[s][g : g + 1] + jnp.sum(
                jnp.where(lane == tp * groups + g, log_gate[s : s + 1], 0.0),
                axis=1,
                keepdims=True,
            )
            own_gate.append(jnp.broadcast_to(gate, (ratio, 1)))
        score_new = score_new - jnp.concatenate(own_gate, axis=0)
        within = jnp.full((n_heads, 1), lengths[s] - 1 - kv * positions, jnp.int32)
        owner = (within >= 0) & (within < positions)
        load_keys[s].wait()
        scores = lax.dot_general(
            spread_q.astype(BF16),
            keys[s],
            (((1,), (1,)), ((), ())),
            preferred_element_type=F32,
        )
        scores = scores + jnp.concatenate(
            [jnp.broadcast_to(bias[s, g : g + 1, :], (ratio, positions)) for g in range(groups)],
            axis=0,
        )
        top = jnp.max(scores, axis=1, keepdims=True)
        top = jnp.maximum(top, jnp.where(owner, score_new, FLOOR))
        weights = jnp.exp(scores - top)
        weight_new = jnp.where(owner, jnp.exp(score_new - top), 0.0)
        weight_new = weight_new.astype(BF16).astype(F32)
        block_sum = jnp.sum(weights, axis=1, keepdims=True) + weight_new
        pick = stat_lane == stat_row + s * n_heads
        max_row = max_row + jnp.sum(jnp.where(pick, top, 0.0), axis=0, keepdims=True)
        sum_row = sum_row + jnp.sum(jnp.where(pick, block_sum, 0.0), axis=0, keepdims=True)
        load_values[s].wait()
        found = jnp.dot(weights.astype(BF16), values[s], preferred_element_type=F32)
        found = jnp.where(own_group, found + weight_new * value_row, 0.0)
        folded = found[:, :LANES]
        for j in range(1, k_rows):
            folded = folded + found[:, j * LANES : (j + 1) * LANES]
        heads_o[s] = folded + swap(folded)
        packed = jnp.where(
            low,
            heads_o[s, pl.ds(0, q_rows, stride=2), :],
            heads_o[s, pl.ds(1, q_rows, stride=2), :],
        )
        blocks[kv, s * q_rows : (s + 1) * q_rows, :] = packed.astype(BF16)
    stats[kv, 0:1, :] = max_row
    stats[kv, 1:2, :] = sum_row
    sent += spread(stats, send_stat, recv_stat)
    sent += spread(blocks, send_block, recv_block)

    arrive(stats, send_stat, recv_stat)
    maxima = [stats[i, 0:1, :] for i in range(n_kv)]
    top = functools.reduce(jnp.maximum, maxima)
    factors = [jnp.exp(m - top) for m in maxima]
    normal = functools.reduce(
        jnp.add, [factors[i] * stats[i, 1:2, :] for i in range(n_kv)]
    )
    pair_row = lax.broadcasted_iota(jnp.int32, (seqs * q_rows, LANES), 0)
    pair_lane = lax.broadcasted_iota(jnp.int32, (seqs * q_rows, LANES), 1)
    shares = []
    for i in range(n_kv):
        share = factors[i] / normal
        first = jnp.sum(jnp.where(pair_lane == 2 * pair_row, share, 0.0), axis=1, keepdims=True)
        second = jnp.sum(
            jnp.where(pair_lane == 2 * pair_row + 1, share, 0.0), axis=1, keepdims=True
        )
        shares.append(jnp.where(low, first, second))
    arrive(blocks, send_block, recv_block)
    attended = shares[0] * blocks[0].astype(F32)
    for i in range(1, n_kv):
        attended = attended + shares[i] * blocks[i].astype(F32)
    mixed_in[...] = attended
    flat = jnp.concatenate(
        [mixed_in[pl.ds(c, seqs, stride=q_rows), :] for c in range(q_rows)], axis=1
    ).astype(BF16)
    load_out.wait()
    mixed = jnp.dot(flat, ow[...], preferred_element_type=F32).astype(BF16)
    halves[tp] = mixed
    for step in range(1, n_tp):
        peer = lax.rem(tp + step, n_tp)
        copy = pltpu.make_async_remote_copy(
            src_ref=halves.at[tp],
            dst_ref=halves.at[tp],
            send_sem=half_sem.at[0, step],
            recv_sem=half_sem.at[1, tp],
            device_id={"tp": peer},
            device_id_type=MESH,
        )
        copy.start()
        sent.append(copy)
    for step in range(1, n_tp):
        peer = lax.rem(tp + n_tp - step, n_tp)
        pltpu.make_async_remote_copy(
            src_ref=halves.at[peer],
            dst_ref=halves.at[peer],
            send_sem=half_sem.at[0, step],
            recv_sem=half_sem.at[1, peer],
            device_id={"tp": peer},
            device_id_type=MESH,
        ).wait_recv()
    result = halves[0].astype(F32)
    for i in range(1, n_tp):
        result = result + halves[i].astype(F32)
    out[...] = result.astype(BF16)
    for copy in sent:
        copy.wait_send()


def per_device(
    n_kv,
    n_tp,
    tokens,
    norm_gain,
    query_weight,
    key_weight,
    value_weight,
    gate_weight,
    gate_bias,
    query_gain,
    key_gain,
    key_cache,
    value_cache,
    gate_cache,
    lengths,
    out_weight,
):
    seqs, columns = tokens.shape
    head = query_gain.shape[0]
    q_width = query_weight.shape[1]
    k_width = key_weight.shape[1]
    n_heads = q_width // head
    q_rows, k_rows = q_width // LANES, k_width // LANES
    used = seqs * (q_rows + 2 * k_rows + 1)
    rows = -(-used // 16) * 16
    any_space = pl.BlockSpec(memory_space=pl.ANY)
    vmem = pl.BlockSpec(memory_space=pltpu.VMEM)
    smem = pl.BlockSpec(memory_space=pltpu.SMEM)
    dma = pltpu.SemaphoreType.DMA
    copies = CHUNKS + 5 + 2 * seqs
    call = pl.pallas_call(
        functools.partial(kernel, (n_kv, n_tp, gate_weight.shape[0], head)),
        out_shape=jax.ShapeDtypeStruct((seqs, out_weight.shape[1]), BF16),
        in_specs=[
            vmem,
            vmem,
            any_space,
            any_space,
            any_space,
            any_space,
            smem,
            vmem,
            vmem,
            any_space,
            any_space,
            any_space,
            smem,
            any_space,
        ],
        out_specs=vmem,
        scratch_shapes=[
            pltpu.VMEM((CHUNKS, columns, q_width // CHUNKS), BF16),
            pltpu.VMEM((columns, k_width), BF16),
            pltpu.VMEM((columns, k_width), BF16),
            pltpu.VMEM((gate_weight.shape[1], columns), BF16),
            pltpu.VMEM(key_cache.shape, BF16),
            pltpu.VMEM(value_cache.shape, BF16),
            pltpu.VMEM(gate_cache.shape, F32),
            pltpu.VMEM(out_weight.shape, BF16),
            pltpu.VMEM((rows, LANES), F32),
            pltpu.VMEM(gate_cache.shape, F32),
            pltpu.VMEM((seqs, n_heads, LANES), F32),
            pltpu.VMEM((seqs, n_heads, LANES), F32),
            pltpu.VMEM((seqs * q_rows, LANES), F32),
            pltpu.VMEM((n_kv, rows, LANES), BF16),
            pltpu.VMEM((n_kv, seqs * q_rows, LANES), BF16),
            pltpu.VMEM((n_kv, 2, LANES), F32),
            pltpu.VMEM((n_tp, seqs, out_weight.shape[1]), BF16),
            dma((copies,)),
            dma((n_kv,)),
            dma((n_kv,)),
            dma((n_kv,)),
            dma((n_kv,)),
            dma((n_kv,)),
            dma((n_kv,)),
            dma((2, n_tp)),
        ],
        compiler_params=pltpu.CompilerParams(
            collective_id=0, has_side_effects=True, vmem_limit_bytes=60 * 1024 * 1024
        ),
    )
    return call(
        tokens,
        norm_gain.reshape(1, columns),
        query_weight,
        key_weight,
        value_weight,
        gate_weight.T,
        gate_bias,
        query_gain.reshape(1, head),
        key_gain.reshape(1, head),
        key_cache,
        value_cache,
        gate_cache,
        lengths,
        out_weight,
    )


def solution(mesh):
    return jax.shard_map(
        functools.partial(per_device, mesh.shape["kv"], mesh.shape["tp"]),
        mesh=mesh,
        in_specs=(
            P("dp", "kv"),
            P("kv"),
            P("kv", "tp"),
            P("kv", "tp"),
            P("kv", "tp"),
            P(),
            P(),
            P(),
            P(),
            P("dp", "kv", "tp"),
            P("dp", "kv", "tp"),
            P("dp", "tp", "kv"),
            P("dp"),
            P("tp", "kv"),
        ),
        out_specs=P("dp", "kv"),
        check_vma=False,
    )
```

```python
import functools

import jax
import jax.numpy as jnp
from jax import lax
from jax.experimental import pallas as pl
from jax.experimental.pallas import tpu as pltpu
from jax.sharding import PartitionSpec as P

EPSILON = 1e-06
FLOOR = -1e30
LANES = 128
CHUNKS = 4
MESH = pl.DeviceIdType.MESH
F32 = jnp.float32
BF16 = jnp.bfloat16


def kernel(
    dims,
    tokens_hbm,
    norm_gain_hbm,
    query_weight,
    key_weight,
    value_weight,
    gate_weight,
    gate_bias_hbm,
    query_gain_hbm,
    key_gain_hbm,
    key_cache,
    value_cache,
    gate_cache,
    lengths_hbm,
    out_weight,
    out,
    tokens,
    norm_gain,
    gate_bias,
    query_gain,
    key_gain,
    lengths,
    qw,
    kw,
    vw,
    gw,
    keys,
    values,
    gates,
    ow,
    part,
    bias,
    heads_q,
    heads_o,
    mixed_in,
    sums,
    blocks,
    stats,
    halves,
    local_sem,
    send_sum,
    recv_sum,
    send_block,
    recv_block,
    send_stat,
    recv_stat,
    half_sem,
):
    n_kv, n_tp, width, head = dims
    kv = lax.axis_index("kv")
    tp = lax.axis_index("tp")
    seqs, columns = tokens.shape
    positions = keys.shape[1]
    q_chunk = qw.shape[2]
    q_rows = query_weight.shape[1] // LANES
    k_width = key_weight.shape[1]
    k_rows = k_width // LANES
    groups = k_width // head
    n_heads = query_weight.shape[1] // head
    ratio = n_heads // groups
    k_base = seqs * q_rows
    v_base = k_base + seqs * k_rows
    g_base = v_base + seqs * k_rows
    gate_columns = gate_weight.shape[0]

    barrier = pltpu.get_barrier_semaphore()
    for step in range(1, n_kv):
        peer = lax.rem(kv + step, n_kv)
        pl.semaphore_signal(barrier, inc=1, device_id={"kv": peer}, device_id_type=MESH)
    for step in range(1, n_tp):
        peer = lax.rem(tp + step, n_tp)
        pl.semaphore_signal(barrier, inc=1, device_id={"tp": peer}, device_id_type=MESH)

    loads = []

    def load(src, dst):
        copy = pltpu.make_async_copy(src, dst, local_sem.at[len(loads)])
        copy.start()
        loads.append(copy)
        return copy

    small = [
        load(tokens_hbm, tokens),
        load(norm_gain_hbm, norm_gain),
        load(lengths_hbm, lengths),
        load(gate_bias_hbm, gate_bias),
        load(query_gain_hbm, query_gain),
        load(key_gain_hbm, key_gain),
    ]
    row_start = pl.multiple_of(kv * columns, LANES)
    load_q = [
        load(query_weight.at[:, pl.ds(i * q_chunk, q_chunk)], qw.at[i]) for i in range(CHUNKS)
    ]
    load_k = load(key_weight, kw)
    load_v = load(value_weight, vw)
    load_g = load(gate_weight.at[:, pl.ds(row_start, columns)], gw)
    load_gates = load(gate_cache, gates)
    load_keys = [load(key_cache.at[s], keys.at[s]) for s in range(seqs)]
    load_values = [load(value_cache.at[s], values.at[s]) for s in range(seqs)]
    load_out = load(out_weight, ow)

    for copy in small:
        copy.wait()
    tokens_f = tokens[...].astype(F32)
    squares = jnp.sum(tokens_f * tokens_f, axis=1, keepdims=True)
    scaled = (tokens_f * norm_gain[...]).astype(BF16)
    for i in range(CHUNKS):
        load_q[i].wait()
        product = jnp.dot(scaled, qw[i], preferred_element_type=F32)
        for j in range(q_chunk // LANES):
            row = i * (q_chunk // LANES) + j
            part[pl.ds(row, seqs, stride=q_rows), :] = product[:, j * LANES : (j + 1) * LANES]
    for copy, weight, base in ((load_k, kw, k_base), (load_v, vw, v_base)):
        copy.wait()
        product = jnp.dot(scaled, weight[...], preferred_element_type=F32)
        for j in range(k_rows):
            part[pl.ds(base + j, seqs, stride=k_rows), :] = product[:, j * LANES : (j + 1) * LANES]
    load_g.wait()
    part[g_base:, :] = jnp.zeros((part.shape[0] - g_base, LANES), F32)
    part[g_base : g_base + seqs, :gate_columns] = lax.dot_general(
        scaled, gw[...], (((1,), (1,)), ((), ())), preferred_element_type=F32
    )
    part[g_base : g_base + seqs, gate_columns : gate_columns + 1] = squares
    sums[kv] = part[...].astype(BF16)

    pl.semaphore_wait(barrier, n_kv + n_tp - 2)

    def spread(ref, send, recv):
        copies = []
        for step in range(1, n_kv):
            peer = lax.rem(kv + step, n_kv)
            copy = pltpu.make_async_remote_copy(
                src_ref=ref.at[kv],
                dst_ref=ref.at[kv],
                send_sem=send.at[step],
                recv_sem=recv.at[kv],
                device_id={"kv": peer},
                device_id_type=MESH,
            )
            copy.start()
            copies.append(copy)
        return copies

    def arrive(ref, send, recv):
        for step in range(1, n_kv):
            peer = lax.rem(kv + n_kv - step, n_kv)
            pltpu.make_async_remote_copy(
                src_ref=ref.at[peer],
                dst_ref=ref.at[peer],
                send_sem=send.at[step],
                recv_sem=recv.at[peer],
                device_id={"kv": peer},
                device_id_type=MESH,
            ).wait_recv()

    sent = spread(sums, send_sum, recv_sum)

    lane = lax.broadcasted_iota(jnp.int32, (1, LANES), 1)
    low = lane < head
    places = lax.broadcasted_iota(jnp.int32, (groups, positions), 1)
    load_gates.wait()
    last_gates = []
    for s in range(seqs):
        within = lengths[s] - 1 - kv * positions
        gate = gates[s]
        bias[s] = jnp.where(places <= within, -gate, FLOOR)
        last_gates.append(
            jnp.sum(jnp.where(places == within, gate, 0.0), axis=1, keepdims=True)
        )
    bias_row = jnp.zeros((1, LANES), F32)
    for j in range(gate_columns):
        bias_row = jnp.where(lane == j, gate_bias[j], bias_row)
    q_gain = jnp.concatenate([query_gain[...]] * (LANES // head), axis=1)
    k_gain = jnp.concatenate([key_gain[...]] * (LANES // head), axis=1)

    def head_norm(raw, gain):
        square = raw * raw
        first = jnp.sum(jnp.where(low, square, 0.0), axis=1, keepdims=True)
        second = jnp.sum(jnp.where(low, 0.0, square), axis=1, keepdims=True)
        factor = jnp.where(
            low, lax.rsqrt(first / head + EPSILON), lax.rsqrt(second / head + EPSILON)
        )
        return (raw * factor * gain).astype(BF16).astype(F32)

    def swap(x):
        return pltpu.roll(x, head, 1)

    head_row = lax.broadcasted_iota(jnp.int32, (n_heads, k_width), 0)
    head_lane = lax.broadcasted_iota(jnp.int32, (n_heads, k_width), 1)
    own_group = (head_row // ratio) == (head_lane // head)
    stat_row = lax.broadcasted_iota(jnp.int32, (n_heads, LANES), 0)
    stat_lane = lax.broadcasted_iota(jnp.int32, (n_heads, LANES), 1)

    for copy in load_keys + load_values + [load_out]:
        copy.wait()
    arrive(sums, send_sum, recv_sum)
    total = sums[0].astype(F32)
    for i in range(1, n_kv):
        total = total + sums[i].astype(F32)
    tail = total[g_base : g_base + seqs]
    square_sum = jnp.sum(jnp.where(lane == gate_columns, tail, 0.0), axis=1, keepdims=True)
    inverse = lax.rsqrt(square_sum / width + EPSILON)
    logits = tail * inverse + bias_row
    log_gate = jnp.minimum(logits, 0.0) - jnp.log1p(jnp.exp(-jnp.abs(logits)))

    max_row = jnp.zeros((1, LANES), F32)
    sum_row = jnp.zeros((1, LANES), F32)
    for s in range(seqs):
        inv = inverse[s : s + 1]
        raw = (total[s * q_rows : (s + 1) * q_rows] * inv).astype(BF16).astype(F32)
        query = head_norm(raw, q_gain) * (head ** -0.5)
        turned = swap(query)
        heads_q[s, pl.ds(0, q_rows, stride=2), :] = jnp.where(low, query, turned)
        heads_q[s, pl.ds(1, q_rows, stride=2), :] = jnp.where(low, turned, query)
        key_raw = total[k_base + s * k_rows : k_base + (s + 1) * k_rows] * inv
        key_new = head_norm(key_raw.astype(BF16).astype(F32), k_gain)
        value_new = (
            (total[v_base + s * k_rows : v_base + (s + 1) * k_rows] * inv)
            .astype(BF16)
            .astype(F32)
        )
        key_row = jnp.concatenate([key_new[j : j + 1] for j in range(k_rows)], axis=1)
        value_row = jnp.concatenate([value_new[j : j + 1] for j in range(k_rows)], axis=1)
        spread_q = jnp.where(
            own_group, jnp.concatenate([heads_q[s]] * k_rows, axis=1), 0.0
        )
        score_new = jnp.sum(spread_q * key_row, axis=1, keepdims=True)
        own_gate = []
        for g in range(groups):
            gate = last_gates[s][g : g + 1] + jnp.sum(
                jnp.where(lane == tp * groups + g, log_gate[s : s + 1], 0.0),
                axis=1,
                keepdims=True,
            )
            own_gate.append(jnp.broadcast_to(gate, (ratio, 1)))
        score_new = score_new - jnp.concatenate(own_gate, axis=0)
        within = jnp.full((n_heads, 1), lengths[s] - 1 - kv * positions, jnp.int32)
        owner = (within >= 0) & (within < positions)
        scores = lax.dot_general(
            spread_q.astype(BF16),
            keys[s],
            (((1,), (1,)), ((), ())),
            preferred_element_type=F32,
        )
        scores = scores + jnp.concatenate(
            [jnp.broadcast_to(bias[s, g : g + 1, :], (ratio, positions)) for g in range(groups)],
            axis=0,
        )
        top = jnp.max(scores, axis=1, keepdims=True)
        top = jnp.maximum(top, jnp.where(owner, score_new, FLOOR))
        weights = jnp.exp(scores - top)
        weight_new = jnp.where(owner, jnp.exp(score_new - top), 0.0)
        weight_new = weight_new.astype(BF16).astype(F32)
        block_sum = jnp.sum(weights, axis=1, keepdims=True) + weight_new
        pick = stat_lane == stat_row + s * n_heads
        max_row = max_row + jnp.sum(jnp.where(pick, top, 0.0), axis=0, keepdims=True)
        sum_row = sum_row + jnp.sum(jnp.where(pick, block_sum, 0.0), axis=0, keepdims=True)
        found = jnp.dot(weights.astype(BF16), values[s], preferred_element_type=F32)
        found = jnp.where(own_group, found + weight_new * value_row, 0.0)
        folded = found[:, :LANES]
        for j in range(1, k_rows):
            folded = folded + found[:, j * LANES : (j + 1) * LANES]
        heads_o[s] = folded + swap(folded)
        packed = jnp.where(
            low,
            heads_o[s, pl.ds(0, q_rows, stride=2), :],
            heads_o[s, pl.ds(1, q_rows, stride=2), :],
        )
        blocks[kv, s * q_rows : (s + 1) * q_rows, :] = packed.astype(BF16)
    stats[kv, 0:1, :] = max_row
    stats[kv, 1:2, :] = sum_row
    sent += spread(stats, send_stat, recv_stat)
    sent += spread(blocks, send_block, recv_block)

    arrive(stats, send_stat, recv_stat)
    maxima = [stats[i, 0:1, :] for i in range(n_kv)]
    top = functools.reduce(jnp.maximum, maxima)
    factors = [jnp.exp(m - top) for m in maxima]
    normal = functools.reduce(
        jnp.add, [factors[i] * stats[i, 1:2, :] for i in range(n_kv)]
    )
    pair_row = lax.broadcasted_iota(jnp.int32, (seqs * q_rows, LANES), 0)
    pair_lane = lax.broadcasted_iota(jnp.int32, (seqs * q_rows, LANES), 1)
    shares = []
    for i in range(n_kv):
        share = factors[i] / normal
        first = jnp.sum(jnp.where(pair_lane == 2 * pair_row, share, 0.0), axis=1, keepdims=True)
        second = jnp.sum(
            jnp.where(pair_lane == 2 * pair_row + 1, share, 0.0), axis=1, keepdims=True
        )
        shares.append(jnp.where(low, first, second))
    arrive(blocks, send_block, recv_block)
    attended = shares[0] * blocks[0].astype(F32)
    for i in range(1, n_kv):
        attended = attended + shares[i] * blocks[i].astype(F32)
    mixed_in[...] = attended
    flat = jnp.concatenate(
        [mixed_in[pl.ds(c, seqs, stride=q_rows), :] for c in range(q_rows)], axis=1
    ).astype(BF16)
    mixed = jnp.dot(flat, ow[...], preferred_element_type=F32).astype(BF16)
    halves[tp] = mixed
    for step in range(1, n_tp):
        peer = lax.rem(tp + step, n_tp)
        copy = pltpu.make_async_remote_copy(
            src_ref=halves.at[tp],
            dst_ref=halves.at[tp],
            send_sem=half_sem.at[0, step],
            recv_sem=half_sem.at[1, tp],
            device_id={"tp": peer},
            device_id_type=MESH,
        )
        copy.start()
        sent.append(copy)
    for step in range(1, n_tp):
        peer = lax.rem(tp + n_tp - step, n_tp)
        pltpu.make_async_remote_copy(
            src_ref=halves.at[peer],
            dst_ref=halves.at[peer],
            send_sem=half_sem.at[0, step],
            recv_sem=half_sem.at[1, peer],
            device_id={"tp": peer},
            device_id_type=MESH,
        ).wait_recv()
    result = halves[0].astype(F32)
    for i in range(1, n_tp):
        result = result + halves[i].astype(F32)
    out[...] = result.astype(BF16)
    for copy in sent:
        copy.wait_send()


def per_device(
    n_kv,
    n_tp,
    tokens,
    norm_gain,
    query_weight,
    key_weight,
    value_weight,
    gate_weight,
    gate_bias,
    query_gain,
    key_gain,
    key_cache,
    value_cache,
    gate_cache,
    lengths,
    out_weight,
):
    seqs, columns = tokens.shape
    head = query_gain.shape[0]
    q_width = query_weight.shape[1]
    k_width = key_weight.shape[1]
    n_heads = q_width // head
    q_rows, k_rows = q_width // LANES, k_width // LANES
    used = seqs * (q_rows + 2 * k_rows + 1)
    rows = -(-used // 16) * 16
    vmem = pl.BlockSpec(memory_space=pltpu.VMEM)
    dma = pltpu.SemaphoreType.DMA
    copies = CHUNKS + 11 + 2 * seqs
    call = pl.pallas_call(
        functools.partial(kernel, (n_kv, n_tp, gate_weight.shape[0], head)),
        out_shape=pltpu.VMEM((seqs, out_weight.shape[1]), BF16),
        in_specs=[pl.BlockSpec(memory_space=pltpu.HBM)] * 14,
        out_specs=vmem,
        scratch_shapes=[
            pltpu.VMEM((seqs, columns), BF16),
            pltpu.VMEM((1, columns), F32),
            pltpu.SMEM(gate_bias.shape, F32),
            pltpu.VMEM((1, head), F32),
            pltpu.VMEM((1, head), F32),
            pltpu.SMEM(lengths.shape, jnp.int32),
            pltpu.VMEM((CHUNKS, columns, q_width // CHUNKS), BF16),
            pltpu.VMEM((columns, k_width), BF16),
            pltpu.VMEM((columns, k_width), BF16),
            pltpu.VMEM((gate_weight.shape[1], columns), BF16),
            pltpu.VMEM(key_cache.shape, BF16),
            pltpu.VMEM(value_cache.shape, BF16),
            pltpu.VMEM(gate_cache.shape, F32),
            pltpu.VMEM(out_weight.shape, BF16),
            pltpu.VMEM((rows, LANES), F32),
            pltpu.VMEM(gate_cache.shape, F32),
            pltpu.VMEM((seqs, n_heads, LANES), F32),
            pltpu.VMEM((seqs, n_heads, LANES), F32),
            pltpu.VMEM((seqs * q_rows, LANES), F32),
            pltpu.VMEM((n_kv, rows, LANES), BF16),
            pltpu.VMEM((n_kv, seqs * q_rows, LANES), BF16),
            pltpu.VMEM((n_kv, 2, LANES), F32),
            pltpu.VMEM((n_tp, seqs, out_weight.shape[1]), BF16),
            dma((copies,)),
            dma((n_kv,)),
            dma((n_kv,)),
            dma((n_kv,)),
            dma((n_kv,)),
            dma((n_kv,)),
            dma((n_kv,)),
            dma((2, n_tp)),
        ],
        compiler_params=pltpu.CompilerParams(
            collective_id=0, has_side_effects=True, vmem_limit_bytes=60 * 1024 * 1024
        ),
    )
    return call(
        tokens,
        norm_gain.reshape(1, columns),
        query_weight,
        key_weight,
        value_weight,
        gate_weight.T,
        gate_bias,
        query_gain.reshape(1, head),
        key_gain.reshape(1, head),
        key_cache,
        value_cache,
        gate_cache,
        lengths,
        out_weight,
    )


def solution(mesh):
    return jax.shard_map(
        functools.partial(per_device, mesh.shape["kv"], mesh.shape["tp"]),
        mesh=mesh,
        in_specs=(
            P("dp", "kv"),
            P("kv"),
            P("kv", "tp"),
            P("kv", "tp"),
            P("kv", "tp"),
            P(),
            P(),
            P(),
            P(),
            P("dp", "kv", "tp"),
            P("dp", "kv", "tp"),
            P("dp", "tp", "kv"),
            P("dp"),
            P("tp", "kv"),
        ),
        out_specs=P("dp", "kv"),
        check_vma=False,
    )
```

```python
import functools

import jax
import jax.numpy as jnp
from jax import lax
from jax.experimental import pallas as pl
from jax.experimental.pallas import tpu as pltpu
from jax.sharding import PartitionSpec as P

EPSILON = 1e-06
FLOOR = -1e30
LANES = 128
CHUNKS = 4
MESH = pl.DeviceIdType.MESH
F32 = jnp.float32
BF16 = jnp.bfloat16


def kernel(
    dims,
    tokens_hbm,
    norm_gain_hbm,
    query_weight,
    key_weight,
    value_weight,
    gate_weight,
    gate_bias_hbm,
    query_gain_hbm,
    key_gain_hbm,
    key_cache,
    value_cache,
    gate_cache,
    lengths_hbm,
    out_weight,
    out,
    tokens,
    norm_gain,
    gate_bias,
    query_gain,
    key_gain,
    lengths,
    qw,
    kw,
    vw,
    gw,
    keys,
    values,
    gates,
    ow,
    part,
    bias,
    heads_q,
    heads_o,
    mixed_in,
    sums,
    blocks,
    stats,
    halves,
    turned_keys,
    local_sem,
    send_sum,
    recv_sum,
    send_block,
    recv_block,
    send_stat,
    recv_stat,
    half_sem,
):
    n_kv, n_tp, width, head = dims
    kv = lax.axis_index("kv")
    tp = lax.axis_index("tp")
    seqs, columns = tokens.shape
    positions = keys.shape[1]
    q_chunk = qw.shape[2]
    q_rows = query_weight.shape[1] // LANES
    k_width = key_weight.shape[1]
    k_rows = k_width // LANES
    groups = k_width // head
    n_heads = query_weight.shape[1] // head
    ratio = n_heads // groups
    k_base = seqs * q_rows
    v_base = k_base + seqs * k_rows
    g_base = v_base + seqs * k_rows
    gate_columns = gate_weight.shape[0]

    barrier = pltpu.get_barrier_semaphore()
    for step in range(1, n_kv):
        peer = lax.rem(kv + step, n_kv)
        pl.semaphore_signal(barrier, inc=1, device_id={"kv": peer}, device_id_type=MESH)
    for step in range(1, n_tp):
        peer = lax.rem(tp + step, n_tp)
        pl.semaphore_signal(barrier, inc=1, device_id={"tp": peer}, device_id_type=MESH)

    loads = []

    def load(src, dst):
        copy = pltpu.make_async_copy(src, dst, local_sem.at[len(loads)])
        copy.start()
        loads.append(copy)
        return copy

    small = [
        load(tokens_hbm, tokens),
        load(norm_gain_hbm, norm_gain),
        load(lengths_hbm, lengths),
        load(gate_bias_hbm, gate_bias),
        load(query_gain_hbm, query_gain),
        load(key_gain_hbm, key_gain),
    ]
    row_start = pl.multiple_of(kv * columns, LANES)
    load_q = [
        load(query_weight.at[:, pl.ds(i * q_chunk, q_chunk)], qw.at[i]) for i in range(CHUNKS)
    ]
    load_k = load(key_weight, kw)
    load_v = load(value_weight, vw)
    load_g = load(gate_weight.at[:, pl.ds(row_start, columns)], gw)
    load_gates = load(gate_cache, gates)
    load_keys = [load(key_cache.at[s], keys.at[s]) for s in range(seqs)]
    load_values = [load(value_cache.at[s], values.at[s]) for s in range(seqs)]
    load_out = load(out_weight, ow)

    for copy in small:
        copy.wait()
    tokens_f = tokens[...].astype(F32)
    squares = jnp.sum(tokens_f * tokens_f, axis=1, keepdims=True)
    scaled = (tokens_f * norm_gain[...]).astype(BF16)
    for i in range(CHUNKS):
        load_q[i].wait()
        product = jnp.dot(scaled, qw[i], preferred_element_type=F32)
        for j in range(q_chunk // LANES):
            row = i * (q_chunk // LANES) + j
            part[pl.ds(row, seqs, stride=q_rows), :] = product[:, j * LANES : (j + 1) * LANES]
    for copy, weight, base in ((load_k, kw, k_base), (load_v, vw, v_base)):
        copy.wait()
        product = jnp.dot(scaled, weight[...], preferred_element_type=F32)
        for j in range(k_rows):
            part[pl.ds(base + j, seqs, stride=k_rows), :] = product[:, j * LANES : (j + 1) * LANES]
    load_g.wait()
    part[g_base:, :] = jnp.zeros((part.shape[0] - g_base, LANES), F32)
    part[g_base : g_base + seqs, :gate_columns] = lax.dot_general(
        scaled, gw[...], (((1,), (1,)), ((), ())), preferred_element_type=F32
    )
    part[g_base : g_base + seqs, gate_columns : gate_columns + 1] = squares
    sums[kv] = part[...].astype(BF16)

    pl.semaphore_wait(barrier, n_kv + n_tp - 2)

    def far_first(step):
        down = n_kv - 1 - step
        down = down - 1 + (down - kv + n_kv - 1) // n_kv
        up = step + (step - kv + n_kv) // n_kv
        upper = (2 * kv) // n_kv
        return down + upper * (up - down)

    def spread(ref, send, recv):
        copies = []
        for step in range(n_kv - 1):
            peer = far_first(step)
            copy = pltpu.make_async_remote_copy(
                src_ref=ref.at[kv],
                dst_ref=ref.at[kv],
                send_sem=send.at[step],
                recv_sem=recv.at[kv],
                device_id={"kv": peer},
                device_id_type=MESH,
            )
            copy.start()
            copies.append(copy)
        return copies

    def arrive(ref, send, recv):
        for step in range(1, n_kv):
            peer = lax.rem(kv + n_kv - step, n_kv)
            pltpu.make_async_remote_copy(
                src_ref=ref.at[peer],
                dst_ref=ref.at[peer],
                send_sem=send.at[step],
                recv_sem=recv.at[peer],
                device_id={"kv": peer},
                device_id_type=MESH,
            ).wait_recv()

    sent = spread(sums, send_sum, recv_sum)

    lane = lax.broadcasted_iota(jnp.int32, (1, LANES), 1)
    low = lane < head
    places = lax.broadcasted_iota(jnp.int32, (groups, positions), 1)
    load_gates.wait()
    last_gates = []
    for s in range(seqs):
        within = lengths[s] - 1 - kv * positions
        gate = gates[s]
        bias[s] = jnp.where(places <= within, -gate, FLOOR)
        last_gates.append(
            jnp.sum(jnp.where(places == within, gate, 0.0), axis=1, keepdims=True)
        )
    bias_row = jnp.zeros((1, LANES), F32)
    for j in range(gate_columns):
        bias_row = jnp.where(lane == j, gate_bias[j], bias_row)
    q_gain = jnp.concatenate([query_gain[...]] * (LANES // head), axis=1)
    k_gain = jnp.concatenate([key_gain[...]] * (LANES // head), axis=1)

    def head_norm(raw, gain):
        square = raw * raw
        first = jnp.sum(jnp.where(low, square, 0.0), axis=1, keepdims=True)
        second = jnp.sum(jnp.where(low, 0.0, square), axis=1, keepdims=True)
        factor = jnp.where(
            low, lax.rsqrt(first / head + EPSILON), lax.rsqrt(second / head + EPSILON)
        )
        return (raw * factor * gain).astype(BF16).astype(F32)

    def swap(x):
        return pltpu.roll(x, head, 1)

    head_row = lax.broadcasted_iota(jnp.int32, (n_heads, k_width), 0)
    head_lane = lax.broadcasted_iota(jnp.int32, (n_heads, k_width), 1)
    own_group = (head_row // ratio) == (head_lane // head)
    stat_row = lax.broadcasted_iota(jnp.int32, (n_heads, LANES), 0)
    stat_lane = lax.broadcasted_iota(jnp.int32, (n_heads, LANES), 1)

    for copy in load_keys + load_values + [load_out]:
        copy.wait()
    for s in range(seqs):
        turned_keys[s] = keys[s].T
    arrive(sums, send_sum, recv_sum)
    total = sums[0].astype(F32)
    for i in range(1, n_kv):
        total = total + sums[i].astype(F32)
    tail = total[g_base : g_base + seqs]
    square_sum = jnp.sum(jnp.where(lane == gate_columns, tail, 0.0), axis=1, keepdims=True)
    inverse = lax.rsqrt(square_sum / width + EPSILON)
    logits = tail * inverse + bias_row
    log_gate = jnp.minimum(logits, 0.0) - jnp.log1p(jnp.exp(-jnp.abs(logits)))

    max_row = jnp.zeros((1, LANES), F32)
    sum_row = jnp.zeros((1, LANES), F32)
    for s in range(seqs):
        inv = inverse[s : s + 1]
        raw = (total[s * q_rows : (s + 1) * q_rows] * inv).astype(BF16).astype(F32)
        query = head_norm(raw, q_gain) * (head ** -0.5)
        turned = swap(query)
        heads_q[s, pl.ds(0, q_rows, stride=2), :] = jnp.where(low, query, turned)
        heads_q[s, pl.ds(1, q_rows, stride=2), :] = jnp.where(low, turned, query)
        key_raw = total[k_base + s * k_rows : k_base + (s + 1) * k_rows] * inv
        key_new = head_norm(key_raw.astype(BF16).astype(F32), k_gain)
        value_new = (
            (total[v_base + s * k_rows : v_base + (s + 1) * k_rows] * inv)
            .astype(BF16)
            .astype(F32)
        )
        key_row = jnp.concatenate([key_new[j : j + 1] for j in range(k_rows)], axis=1)
        value_row = jnp.concatenate([value_new[j : j + 1] for j in range(k_rows)], axis=1)
        spread_q = jnp.where(
            own_group, jnp.concatenate([heads_q[s]] * k_rows, axis=1), 0.0
        )
        score_new = jnp.sum(spread_q * key_row, axis=1, keepdims=True)
        own_gate = []
        for g in range(groups):
            gate = last_gates[s][g : g + 1] + jnp.sum(
                jnp.where(lane == tp * groups + g, log_gate[s : s + 1], 0.0),
                axis=1,
                keepdims=True,
            )
            own_gate.append(jnp.broadcast_to(gate, (ratio, 1)))
        score_new = score_new - jnp.concatenate(own_gate, axis=0)
        within = jnp.full((n_heads, 1), lengths[s] - 1 - kv * positions, jnp.int32)
        owner = (within >= 0) & (within < positions)
        scores = jnp.dot(
            spread_q.astype(BF16), turned_keys[s], preferred_element_type=F32
        )
        scores = scores + jnp.concatenate(
            [jnp.broadcast_to(bias[s, g : g + 1, :], (ratio, positions)) for g in range(groups)],
            axis=0,
        )
        top = jnp.max(scores, axis=1, keepdims=True)
        top = jnp.maximum(top, jnp.where(owner, score_new, FLOOR))
        weights = jnp.exp(scores - top)
        weight_new = jnp.where(owner, jnp.exp(score_new - top), 0.0)
        weight_new = weight_new.astype(BF16).astype(F32)
        block_sum = jnp.sum(weights, axis=1, keepdims=True) + weight_new
        pick = stat_lane == stat_row + s * n_heads
        max_row = max_row + jnp.sum(jnp.where(pick, top, 0.0), axis=0, keepdims=True)
        sum_row = sum_row + jnp.sum(jnp.where(pick, block_sum, 0.0), axis=0, keepdims=True)
        found = jnp.dot(weights.astype(BF16), values[s], preferred_element_type=F32)
        found = jnp.where(own_group, found + weight_new * value_row, 0.0)
        folded = found[:, :LANES]
        for j in range(1, k_rows):
            folded = folded + found[:, j * LANES : (j + 1) * LANES]
        heads_o[s] = folded + swap(folded)
        packed = jnp.where(
            low,
            heads_o[s, pl.ds(0, q_rows, stride=2), :],
            heads_o[s, pl.ds(1, q_rows, stride=2), :],
        )
        blocks[kv, s * q_rows : (s + 1) * q_rows, :] = packed.astype(BF16)
    stats[kv, 0:1, :] = max_row
    stats[kv, 1:2, :] = sum_row
    sent += spread(stats, send_stat, recv_stat)
    sent += spread(blocks, send_block, recv_block)

    arrive(stats, send_stat, recv_stat)
    maxima = [stats[i, 0:1, :] for i in range(n_kv)]
    top = functools.reduce(jnp.maximum, maxima)
    factors = [jnp.exp(m - top) for m in maxima]
    normal = functools.reduce(
        jnp.add, [factors[i] * stats[i, 1:2, :] for i in range(n_kv)]
    )
    pair_row = lax.broadcasted_iota(jnp.int32, (seqs * q_rows, LANES), 0)
    pair_lane = lax.broadcasted_iota(jnp.int32, (seqs * q_rows, LANES), 1)
    shares = []
    for i in range(n_kv):
        share = factors[i] / normal
        first = jnp.sum(jnp.where(pair_lane == 2 * pair_row, share, 0.0), axis=1, keepdims=True)
        second = jnp.sum(
            jnp.where(pair_lane == 2 * pair_row + 1, share, 0.0), axis=1, keepdims=True
        )
        shares.append(jnp.where(low, first, second))
    arrive(blocks, send_block, recv_block)
    attended = shares[0] * blocks[0].astype(F32)
    for i in range(1, n_kv):
        attended = attended + shares[i] * blocks[i].astype(F32)
    mixed_in[...] = attended
    flat = jnp.concatenate(
        [mixed_in[pl.ds(c, seqs, stride=q_rows), :] for c in range(q_rows)], axis=1
    ).astype(BF16)
    mixed = jnp.dot(flat, ow[...], preferred_element_type=F32).astype(BF16)
    halves[tp] = mixed
    for step in range(1, n_tp):
        peer = lax.rem(tp + step, n_tp)
        copy = pltpu.make_async_remote_copy(
            src_ref=halves.at[tp],
            dst_ref=halves.at[tp],
            send_sem=half_sem.at[0, step],
            recv_sem=half_sem.at[1, tp],
            device_id={"tp": peer},
            device_id_type=MESH,
        )
        copy.start()
        sent.append(copy)
    for step in range(1, n_tp):
        peer = lax.rem(tp + n_tp - step, n_tp)
        pltpu.make_async_remote_copy(
            src_ref=halves.at[peer],
            dst_ref=halves.at[peer],
            send_sem=half_sem.at[0, step],
            recv_sem=half_sem.at[1, peer],
            device_id={"tp": peer},
            device_id_type=MESH,
        ).wait_recv()
    result = halves[0].astype(F32)
    for i in range(1, n_tp):
        result = result + halves[i].astype(F32)
    out[...] = result.astype(BF16)
    for copy in sent:
        copy.wait_send()


def per_device(
    n_kv,
    n_tp,
    tokens,
    norm_gain,
    query_weight,
    key_weight,
    value_weight,
    gate_weight,
    gate_bias,
    query_gain,
    key_gain,
    key_cache,
    value_cache,
    gate_cache,
    lengths,
    out_weight,
):
    seqs, columns = tokens.shape
    head = query_gain.shape[0]
    q_width = query_weight.shape[1]
    k_width = key_weight.shape[1]
    n_heads = q_width // head
    q_rows, k_rows = q_width // LANES, k_width // LANES
    used = seqs * (q_rows + 2 * k_rows + 1)
    rows = -(-used // 8) * 8
    vmem = pl.BlockSpec(memory_space=pltpu.VMEM)
    dma = pltpu.SemaphoreType.DMA
    copies = CHUNKS + 11 + 2 * seqs
    call = pl.pallas_call(
        functools.partial(kernel, (n_kv, n_tp, gate_weight.shape[0], head)),
        out_shape=pltpu.VMEM((seqs, out_weight.shape[1]), BF16),
        in_specs=[pl.BlockSpec(memory_space=pltpu.HBM)] * 14,
        out_specs=vmem,
        scratch_shapes=[
            pltpu.VMEM((seqs, columns), BF16),
            pltpu.VMEM((1, columns), F32),
            pltpu.SMEM(gate_bias.shape, F32),
            pltpu.VMEM((1, head), F32),
            pltpu.VMEM((1, head), F32),
            pltpu.SMEM(lengths.shape, jnp.int32),
            pltpu.VMEM((CHUNKS, columns, q_width // CHUNKS), BF16),
            pltpu.VMEM((columns, k_width), BF16),
            pltpu.VMEM((columns, k_width), BF16),
            pltpu.VMEM((gate_weight.shape[1], columns), BF16),
            pltpu.VMEM(key_cache.shape, BF16),
            pltpu.VMEM(value_cache.shape, BF16),
            pltpu.VMEM(gate_cache.shape, F32),
            pltpu.VMEM(out_weight.shape, BF16),
            pltpu.VMEM((rows, LANES), F32),
            pltpu.VMEM(gate_cache.shape, F32),
            pltpu.VMEM((seqs, n_heads, LANES), F32),
            pltpu.VMEM((seqs, n_heads, LANES), F32),
            pltpu.VMEM((seqs * q_rows, LANES), F32),
            pltpu.VMEM((n_kv, rows, LANES), BF16),
            pltpu.VMEM((n_kv, seqs * q_rows, LANES), BF16),
            pltpu.VMEM((n_kv, 2, LANES), F32),
            pltpu.VMEM((n_tp, seqs, out_weight.shape[1]), BF16),
            pltpu.VMEM((seqs, key_cache.shape[2], key_cache.shape[1]), BF16),
            dma((copies,)),
            dma((n_kv,)),
            dma((n_kv,)),
            dma((n_kv,)),
            dma((n_kv,)),
            dma((n_kv,)),
            dma((n_kv,)),
            dma((2, n_tp)),
        ],
        compiler_params=pltpu.CompilerParams(
            collective_id=0, has_side_effects=True, vmem_limit_bytes=60 * 1024 * 1024
        ),
    )
    return call(
        tokens,
        norm_gain.reshape(1, columns),
        query_weight,
        key_weight,
        value_weight,
        gate_weight.T,
        gate_bias,
        query_gain.reshape(1, head),
        key_gain.reshape(1, head),
        key_cache,
        value_cache,
        gate_cache,
        lengths,
        out_weight,
    )


def solution(mesh):
    return jax.shard_map(
        functools.partial(per_device, mesh.shape["kv"], mesh.shape["tp"]),
        mesh=mesh,
        in_specs=(
            P("dp", "kv"),
            P("kv"),
            P("kv", "tp"),
            P("kv", "tp"),
            P("kv", "tp"),
            P(),
            P(),
            P(),
            P(),
            P("dp", "kv", "tp"),
            P("dp", "kv", "tp"),
            P("dp", "tp", "kv"),
            P("dp"),
            P("tp", "kv"),
        ),
        out_specs=P("dp", "kv"),
        check_vma=False,
    )
```
